256 devices in a mesh: grp: 2 (over y), sp: 16 (over z), fs: 4 (over x), tp: 2 (over core).
Axes of the slice: x: 4, y: 2, z: 16, core: 2. Of those that a mesh axis runs over, the one named last changes fastest.
The devices are a block of a 4x16x16 slice.
Arguments:
- tokens: bfloat16 [8, 2048, 2048], P(('grp', 'fs'), 'sp'), parts along dimension 0, may hold values from -6 to 6
- norm_gain: float32 [2048], replicated, may hold values from 0.1 to 1.9
- query_attend: bfloat16 [2048, 8, 128], P(None, ('fs', 'tp')), may hold values from -0.125 to 0.125
- key_attend: bfloat16 [2048, 8, 128], P(None, ('fs', 'tp')), may hold values from -0.125 to 0.125
- value_attend: bfloat16 [2048, 8, 128], P(None, ('fs', 'tp')), may hold values from -0.125 to 0.125
- query_linear: bfloat16 [2048, 8, 128], P(None, ('fs', 'tp')), may hold values from -0.125 to 0.125
- key_linear: bfloat16 [2048, 8, 128], P(None, ('fs', 'tp')), may hold values from -0.125 to 0.125
- value_linear: bfloat16 [2048, 8, 256], P(None, ('fs', 'tp')), may hold values from -0.125 to 0.125
- decay_down: bfloat16 [2048, 32], replicated, may hold values from -0.125 to 0.125
- decay_up: bfloat16 [32, 8, 128], replicated, may hold values from -2.109375 to 2.109375
- decay_bias: float32 [8, 128], replicated, may hold values from -1.5 to 7.5
- log_retain: float32 [8, 2048, 8], P(('grp', 'fs'), 'sp'), parts along dimension 0, may hold values from -1.5 to 0
- query_gain: float32 [64], replicated, may hold values from 0.6 to 4
- key_gain: float32 [8, 2, 64], replicated, may hold values from 0.8 to 14
- diff_lambda: float32 [8], replicated, may hold values from 0.3 to 0.8
- mix_gain: float32 [128], replicated, may hold values from 0.1 to 1.9
- state_gain: float32 [256], replicated, may hold values from 0.1 to 1.9
- init_state: float32 [8, 8, 128, 256], P('grp', ('fs', 'tp')), parts along dimension 0, may hold values from -160 to 160
- output_attend: bfloat16 [1024, 2048], P(None, 'tp'), may hold values from -0.109375 to 0.109375
- output_linear: bfloat16 [2048, 2048], P(None, 'tp'), may hold values from -0.109375 to 0.109375
Outputs:
- mixed_out: bfloat16 [8, 2048, 2048], P(('grp', 'fs'), 'sp', 'tp'), parts along dimension 0
The draws below stay inside these ranges and needn't reach their ends.
There are 2 independent parts, one for each index of `grp`. The reference program is written for one: setup_inputs(seed, part) draws one part's arguments, and reference() takes and returns one part's arrays. A program takes and returns all parts, laid end to end along the dimension named above; an argument that names none is the same for every part. Nothing has to cross between parts.
All inputs are finite; a program needn't handle non-finite values.
Results may differ from the reference program's by a relative error of at most 0.018.
The reference program's roundings to bfloat16 on the way count: a program that leaves them out, or rounds other values in their place, can miss the bound.
Values may be sent and summed in bfloat16 or wider, within the bound.
A program may use at most 128 MiB of HBM per device.

```python
import math
import jax
import jax.numpy as jnp
from jax import lax

D = 2048
MIXER_HEADS = 8
HD_A = 64
DV_A = 128
HDK = 128
HDV = 256
RANK = 32
BLK = 64
TOK_DEV = 128
SEQUENCE_LENGTH = 2048
SEQUENCE_COUNT = 4
N_SP = 16


def draw_query_gain(key, part):
    return jax.random.uniform(key, (HD_A,), jnp.float32, 0.6, 2.0)


def draw_key_gain(key, part):
    level_key = jax.random.fold_in(key, 11)
    channel_key = jax.random.fold_in(key, 12)
    level = jax.random.uniform(level_key, (MIXER_HEADS, 2, 1), jnp.float32, 1.2, 1.6)
    return level * jax.random.uniform(channel_key, (MIXER_HEADS, 2, HD_A), jnp.float32, 0.85, 1.15)


def draw_decay_bias(key, part):
    pick_key = jax.random.fold_in(key, 21)
    fast_key = jax.random.fold_in(key, 22)
    slow_key = jax.random.fold_in(key, 23)
    share = 0.5
    fast_pick = jax.random.uniform(pick_key, (MIXER_HEADS, HDK), jnp.float32) < share
    fast_value = jax.random.uniform(fast_key, (MIXER_HEADS, HDK), jnp.float32, -1.5, 0.5)
    slow_value = jax.random.uniform(slow_key, (MIXER_HEADS, HDK), jnp.float32, 6.0, 7.5)
    return jnp.where(fast_pick, fast_value, slow_value)


def draw_log_retain(key, part):
    rate_key = jax.random.fold_in(key, 31)
    spot_key = jax.random.fold_in(key, 32)
    random_depth_key = jax.random.fold_in(key, 33)
    block_total = SEQUENCE_LENGTH // TOK_DEV
    factor = jnp.exp(jax.random.uniform(rate_key, (SEQUENCE_COUNT, block_total, 1, MIXER_HEADS), jnp.float32, math.log(0.5), math.log(2.0)))
    position_offset = jnp.broadcast_to(-0.8 / SEQUENCE_LENGTH * factor, (SEQUENCE_COUNT, block_total, TOK_DEV, MIXER_HEADS)).reshape(SEQUENCE_COUNT, SEQUENCE_LENGTH, MIXER_HEADS)
    spike_positions = jax.random.randint(spot_key, (SEQUENCE_COUNT, 1, MIXER_HEADS, 2), 0, SEQUENCE_LENGTH)
    spike_depth = jnp.log(jax.random.uniform(random_depth_key, (SEQUENCE_COUNT, 1, MIXER_HEADS, 2), jnp.float32, 0.5, 0.8))
    spike_location = jnp.arange(SEQUENCE_LENGTH, dtype=jnp.int32)[None, :, None, None] == spike_positions
    spike_total = jnp.sum(jnp.where(spike_location, spike_depth, 0.0), axis=-1)
    return position_offset + spike_total


def shard_levels(key, extent, shards, smallest, high):
    loudness, own = 1.0, jax.random.fold_in(key, 6)
    for dim, blocks in shards:
        draws = jnp.exp(jax.random.uniform(jax.random.fold_in(own, dim), (blocks,), jnp.float32, smallest / len(shards), high / len(shards)))
        loudness = loudness * jnp.repeat(draws, extent[dim] // blocks).reshape([-1 if axis == dim else 1 for axis in range(len(extent))])
    return loudness


def normal_values(own_key, shape, width, reach, split=(), kind=jnp.bfloat16):
    result = jax.random.normal(own_key, shape, jnp.float32) * width
    if len(split) > 0:
        result = shard_levels(own_key, shape, split, -0.22, 0.18) * result
    return jnp.clip(result, min=-reach, max=reach).astype(kind)


def setup_inputs(seed: int = 0, part: int = 0) -> dict:
    arg_keys = jax.random.split(jax.random.key(seed), 21)
    part_splits = jax.random.split(jax.random.fold_in(arg_keys[20], part), 21)
    tokens = normal_values(part_splits[0], (SEQUENCE_COUNT, SEQUENCE_LENGTH, D), 1.0, 6.0, ((0, 4), (1, 16)))
    norm_gain = jnp.clip(1.0 + 0.18 * jax.random.normal(arg_keys[1], (D,), jnp.float32), 0.1, 1.9)
    query_attend = normal_values(arg_keys[2], (D, MIXER_HEADS, 2 * HD_A), D ** -0.5, 0.125, ((1, 8),))
    key_attend = normal_values(arg_keys[3], (D, MIXER_HEADS, 2 * HD_A), D ** -0.5, 0.125, ((1, 8),))
    value_attend = normal_values(arg_keys[4], (D, MIXER_HEADS, DV_A), D ** -0.5, 0.125, ((1, 8),))
    query_linear = normal_values(arg_keys[5], (D, MIXER_HEADS, HDK), D ** -0.5, 0.125, ((1, 8),))
    key_linear = normal_values(arg_keys[6], (D, MIXER_HEADS, HDK), D ** -0.5, 0.125, ((1, 8),))
    value_linear = normal_values(arg_keys[7], (D, MIXER_HEADS, HDV), D ** -0.5, 0.125, ((1, 8),))
    decay_down = normal_values(arg_keys[8], (D, RANK), D ** -0.5, 0.125)
    decay_up = normal_values(arg_keys[9], (RANK, MIXER_HEADS, HDK), (2.0 / RANK ** 0.5), 2.109375)
    decay_bias = draw_decay_bias(jax.random.fold_in(arg_keys[20], 71), part)
    log_retain = draw_log_retain(jax.random.fold_in(jax.random.fold_in(arg_keys[20], part), 71), part)
    query_gain = draw_query_gain(jax.random.fold_in(arg_keys[20], 71), part)
    key_gain = draw_key_gain(jax.random.fold_in(arg_keys[20], 71), part)
    diff_lambda = jnp.clip(jax.random.uniform(arg_keys[14], (MIXER_HEADS,), jnp.float32, 0.3, 0.8), 0.3, 0.8)
    mix_gain = jnp.clip(1.0 + 0.18 * jax.random.normal(arg_keys[15], (DV_A,), jnp.float32), 0.1, 1.9)
    state_gain = jnp.clip(1.0 + 0.18 * jax.random.normal(arg_keys[16], (HDV,), jnp.float32), 0.1, 1.9)
    init_state = normal_values(part_splits[17], (SEQUENCE_COUNT, MIXER_HEADS, HDK, HDV), (0.6 * (TOK_DEV * N_SP) ** 0.5), 160.0, ((1, 8),), jnp.float32)
    output_attend = normal_values(arg_keys[18], (MIXER_HEADS * DV_A, D), (MIXER_HEADS * (DV_A + HDV)) ** -0.5, 0.109375, ((1, 2),))
    output_linear = normal_values(arg_keys[19], (MIXER_HEADS * HDV, D), (MIXER_HEADS * (DV_A + HDV)) ** -0.5, 0.109375, ((1, 2),))
    return dict(tokens=tokens, norm_gain=norm_gain, query_attend=query_attend, key_attend=key_attend, value_attend=value_attend, query_linear=query_linear, key_linear=key_linear, value_linear=value_linear, decay_down=decay_down, decay_up=decay_up, decay_bias=decay_bias, log_retain=log_retain, query_gain=query_gain, key_gain=key_gain, diff_lambda=diff_lambda, mix_gain=mix_gain, state_gain=state_gain, init_state=init_state, output_attend=output_attend, output_linear=output_linear)


norm_eps = 1e-06
decay_tau = 16.0

def rms_scale(values, gain):
    widened = values.astype(jnp.float32)
    return widened * lax.rsqrt(lax.optimization_barrier(jnp.mean(widened * widened, axis=-1, keepdims=True)) + norm_eps) * gain

def widen(values):
    return lax.optimization_barrier(values).astype(jnp.float32)

def gated_linear(queries, keys_in, values_in, log_decay, first_state):
    length, head_count, key_dim = queries.shape
    block_count = length // BLK
    highest_precision = lax.Precision.HIGHEST

    def split_blocks(source):
        return source.reshape(block_count, BLK, head_count, source.shape[-1])
    causal = (jnp.arange(BLK, dtype=jnp.int32)[:, None] >= jnp.arange(BLK, dtype=jnp.int32)[None, :])[None]

    def advance(recurrent_state, inputs_now):
        question_patch_lines, block_k, value_tile_width, block_log = inputs_now
        running_state = jnp.cumsum(block_log, axis=0)
        pivot = running_state[BLK // 2]
        q_scaled = question_patch_lines * jnp.exp(running_state - pivot[None])
        k_scaled = block_k * jnp.exp(pivot[None] - running_state)
        scores = jnp.einsum('thk,shk->hts', q_scaled, k_scaled, precision=highest_precision)
        scores = jnp.where(causal, scores, 0.0)
        inside_block = jnp.einsum('hts,shv->thv', scores, value_tile_width, precision=highest_precision)
        inside_block = inside_block + jnp.einsum('jwo,wos->jws', question_patch_lines * jnp.exp(running_state), recurrent_state, precision=highest_precision)
        final_state = running_state[-1]
        faded_memory_matrix = block_k * jnp.exp(final_state[None] - running_state)
        recurrent_state = recurrent_state * jnp.exp(final_state)[:, :, None] + jnp.einsum('zcb,zcw->cbw', faded_memory_matrix, value_tile_width, precision=highest_precision)
        return (recurrent_state, inside_block)
    _, outputs = lax.scan(advance, first_state, (split_blocks(queries), split_blocks(keys_in), split_blocks(values_in), split_blocks(log_decay)))
    return outputs.reshape(length, head_count, values_in.shape[-1])

def reference(tokens, norm_gain, query_attend, key_attend, value_attend, query_linear, key_linear, value_linear, decay_down, decay_up, decay_bias, log_retain, query_gain, key_gain, diff_lambda, mix_gain, state_gain, init_state, output_attend, output_linear):

    def one_sequence(inputs_now):
        seq_tokens, seq_retain, seq_state = inputs_now
        seq_len = seq_tokens.shape[0]
        normed = rms_scale(seq_tokens, norm_gain).astype(jnp.bfloat16)

        def project(weight):
            return jnp.dot(normed, weight.reshape(weight.shape[0], -1), preferred_element_type=jnp.float32).astype(jnp.bfloat16)
        q_unit = rms_scale(project(query_attend).reshape(seq_len, MIXER_HEADS, 2, HD_A), query_gain).astype(jnp.bfloat16)
        k_unit = rms_scale(project(key_attend).reshape(seq_len, MIXER_HEADS, 2, HD_A), key_gain).astype(jnp.bfloat16)
        v_attend = project(value_attend).reshape(seq_len, MIXER_HEADS, DV_A)
        key_wide = widen(k_unit)
        value_wide = widen(v_attend)
        position_block = jnp.arange(seq_len, dtype=jnp.int32) // BLK

        def attend(block_index):
            first_row = (block_index * TOK_DEV).astype(jnp.int32)
            query_rows = widen(lax.dynamic_slice_in_dim(q_unit, first_row, TOK_DEV, 0))
            query_block = lax.dynamic_slice_in_dim(position_block, first_row, TOK_DEV, 0)
            scores = jnp.einsum('qhmd,khmd->hmqk', query_rows, key_wide) * HD_A ** (-0.5)
            allowed = query_block[:, None] >= position_block[None, :]
            scores = jnp.where(allowed, scores, -jnp.inf)
            top = lax.optimization_barrier(jnp.max(scores, axis=-1, keepdims=True))
            raised = jnp.exp(scores - top)
            totals = lax.optimization_barrier(jnp.sum(raised, axis=-1))
            sums = jnp.einsum('hmqk,khv->hmqv', widen(raised.astype(jnp.bfloat16)), value_wide)
            return sums[:, 0] / totals[:, 0, :, None] - diff_lambda[:, None, None] * sums[:, 1] / totals[:, 1, :, None]
        diff_raw = lax.map(attend, jnp.arange(seq_len // TOK_DEV, dtype=jnp.int32))
        diff_raw = jnp.transpose(diff_raw, (0, 2, 1, 3)).reshape(seq_len, MIXER_HEADS, DV_A)
        attend_out = rms_scale(diff_raw, mix_gain).astype(jnp.bfloat16)
        q_lin = project(query_linear).reshape(seq_len, MIXER_HEADS, HDK)
        k_lin = project(key_linear).reshape(seq_len, MIXER_HEADS, HDK)
        v_lin = project(value_linear).reshape(seq_len, MIXER_HEADS, HDV)
        low_rank = jnp.dot(normed, decay_down, preferred_element_type=jnp.float32).astype(jnp.bfloat16)
        pre_act = jnp.dot(low_rank, decay_up.reshape(RANK, -1), preferred_element_type=jnp.float32).reshape(seq_len, MIXER_HEADS, HDK) + decay_bias
        log_decay = jax.nn.log_sigmoid(pre_act) / decay_tau + seq_retain[:, :, None]
        linear_raw = gated_linear(widen(q_lin) * HDK ** (-0.5), widen(k_lin), widen(v_lin), log_decay, seq_state)
        linear_out = rms_scale(linear_raw, state_gain).astype(jnp.bfloat16)
        total = jnp.dot(attend_out.reshape(seq_len, -1), output_attend, preferred_element_type=jnp.float32)
        total = total + jnp.dot(linear_out.reshape(seq_len, -1), output_linear, preferred_element_type=jnp.float32)
        return total.astype(jnp.bfloat16)
    return lax.map(one_sequence, (tokens, log_retain, init_state))
```

```python
import functools

import jax
import jax.numpy as jnp
from jax import lax
from jax.experimental import pallas as pl
from jax.experimental.pallas import tpu as pltpu
from jax.sharding import PartitionSpec as P

HEADS = 8
HALF = 64
HD = 128
HV = 256
BLK = 64
RANK = 32
EPS = 1e-06
TAU = 16.0
MESH = pl.DeviceIdType.MESH
F32 = jnp.float32
BF16 = jnp.bfloat16
NT = (((1,), (1,)), ((), ()))
TN = (((0,), (0,)), ((), ()))
CHAIN_FIRST_UP_TO = 8


def dot(a, b, dims=(((1,), (0,)), ((), ())), **kw):
    return lax.dot_general(a, b, dims, preferred_element_type=F32, **kw)


def iota(shape, dim):
    return lax.broadcasted_iota(jnp.int32, shape, dim)


def turned(row, n):
    return jnp.transpose(jnp.broadcast_to(row, (n, row.shape[-1])))


def unit_norm(x, gain):
    left = iota(x.shape, 1) < HALF
    sq = x * x
    a = jnp.sum(jnp.where(left, sq, 0.0), axis=1, keepdims=True)
    b = jnp.sum(jnp.where(left, 0.0, sq), axis=1, keepdims=True)
    mean = jnp.where(left, a, b) * (1.0 / HALF)
    return (x * lax.rsqrt(mean + EPS) * gain).astype(BF16)


def project_kernel(
    tok_ref,
    gain_ref,
    wqa,
    wka,
    wva,
    wql,
    wkl,
    wvl,
    down_ref,
    up_ref,
    bias_ref,
    retain_ref,
    qgain_ref,
    kgain_ref,
    kv_out,
    q_out,
    qr_out,
    inside_out,
    local_out,
    decay_out,
    weights,
    gath,
    rets,
    w_sem,
    send,
    recv,
    r_send,
    r_recv,
):
    x = lax.axis_index("fs")
    t = lax.axis_index("tp")
    n = lax.axis_size("fs")
    right, left, far = lax.rem(x + 1, n), lax.rem(x + n - 1, n), lax.rem(x + 2, n)
    head = x * 2 + t
    rows = tok_ref.shape[0]

    copies = []
    at = 0
    for i, w in enumerate((wqa, wka, wva, wql, wkl, wvl)):
        width = w.shape[1]
        copies.append(
            pltpu.make_async_copy(w, weights.at[:, pl.ds(at, width)], w_sem.at[i])
        )
        at += width
    for c in copies:
        c.start()

    barrier = pltpu.get_barrier_semaphore()
    for peer in (left, right, far):
        pl.semaphore_signal(barrier, inc=1, device_id={"fs": peer}, device_id_type=MESH)
    pl.semaphore_signal(barrier, inc=1, device_id={"tp": 1 - t}, device_id_type=MESH)

    gain = gain_ref[...]

    def normalize(start):
        part = tok_ref[pl.ds(start, 32), :].astype(F32)
        mean = jnp.mean(part * part, axis=1, keepdims=True)
        gath[0, pl.ds(start, 32), :] = (part * lax.rsqrt(mean + EPS) * gain).astype(BF16)

    lo = pl.multiple_of(t * 64, 64)
    hi = pl.multiple_of(t * 64 + 32, 32)
    other = pl.multiple_of((1 - t) * 64, 64)
    other_hi = pl.multiple_of((1 - t) * 64 + 32, 32)
    rets[0] = retain_ref[...]
    normalize(lo)
    normalize(hi)
    pl.semaphore_wait(barrier, 4)

    def remote(i, slot_from, slot_to, start, peer):
        return pltpu.make_async_remote_copy(
            src_ref=gath.at[slot_from, pl.ds(start, 32), :],
            dst_ref=gath.at[slot_to, pl.ds(start, 32), :],
            send_sem=send.at[i],
            recv_sem=recv.at[i],
            device_id=peer,
            device_id_type=MESH,
        )

    to_right = {"fs": right}
    to_left = {"fs": left}
    partner = {"tp": 1 - t}
    r0 = remote(0, 0, 1, lo, to_right)
    l1 = remote(1, 0, 3, hi, to_left)
    r1 = remote(2, 0, 1, hi, to_right)
    l0 = remote(3, 0, 3, lo, to_left)
    for c in (r0, l1, r1, l0):
        c.start()
    small = []
    for i, (slot, peer) in enumerate(((1, right), (3, left), (2, far))):
        small.append(
            pltpu.make_async_remote_copy(
                src_ref=rets.at[0],
                dst_ref=rets.at[slot],
                send_sem=r_send.at[i],
                recv_sem=r_recv.at[i],
                device_id={"fs": peer},
                device_id_type=MESH,
            )
        )
    for c in small:
        c.start()
    normalize(other)
    normalize(other_hi)
    for c in copies:
        c.wait()

    up_rows = up_ref[...]
    pick = (iota((RANK, RANK * HEADS), 1) == iota((RANK, RANK * HEADS), 0) * HEADS + head)
    pick = jnp.where(pick, 1.0, 0.0).astype(BF16)
    bias = bias_ref[pl.ds(head, 1), :]
    qg = qgain_ref[...]
    qgain = jnp.concatenate([qg, qg], axis=1)
    kg = kgain_ref[pl.ds(head, 1)][0]
    kgain = jnp.concatenate([kg[0:1], kg[1:2]], axis=1)
    rr, cc = iota((rows, rows), 0), iota((rows, rows), 1)
    same = (rr // BLK) == (cc // BLK)
    tri = jnp.where(same & (rr >= cc), 1.0, 0.0)
    second = iota((rows, HD), 0) >= BLK

    def finish(slot, seq):
        act = gath[slot]
        got = dot(act, weights[...]).astype(BF16)
        low = dot(act, down_ref[...], NT).astype(BF16)
        pre = dot(dot(low, pick).astype(BF16), up_rows) + bias
        log_sig = jnp.minimum(pre, 0.0) - jnp.log1p(jnp.exp(-jnp.abs(pre)))
        keep = jnp.sum(
            jnp.where(iota((HEADS, rows), 0) == head, rets[slot], 0.0), axis=0, keepdims=True
        )
        log_decay = log_sig * (1.0 / TAU) + turned(keep, HD)
        run = dot(tri, log_decay, precision=lax.Precision.HIGHEST)
        q_unit = unit_norm(got[:, 0:HD].astype(F32), qgain)
        k_unit = unit_norm(got[:, HD : 2 * HD].astype(F32), kgain)
        kv_out[seq, :, 0:HD] = k_unit
        kv_out[seq, :, HD : 2 * HD] = got[:, 2 * HD : 3 * HD]
        q_out[seq] = (q_unit.astype(F32) * (HALF**-0.5)).astype(BF16)
        q_lin = got[:, 3 * HD : 4 * HD].astype(F32) * (HD**-0.5)
        k_lin = got[:, 4 * HD : 5 * HD].astype(F32)
        v_lin = got[:, 5 * HD :]
        pivot = jnp.where(second, run[BLK + BLK // 2 : BLK + BLK // 2 + 1], run[BLK // 2 : BLK // 2 + 1])
        end0, end1 = run[BLK - 1 : BLK], run[2 * BLK - 1 : 2 * BLK]
        ends = jnp.where(second, end1, end0)
        scores = dot(
            (q_lin * jnp.exp(run - pivot)).astype(BF16),
            (k_lin * jnp.exp(pivot - run)).astype(BF16),
            NT,
        )
        q_here = q_lin * jnp.exp(run)
        k_left = k_lin * jnp.exp(ends - run)
        across = dot(q_here.astype(BF16), k_left.astype(BF16), NT)
        later = (rr >= BLK) & (cc < BLK)
        mixed = jnp.where(same & (rr >= cc), scores, jnp.where(later, across, 0.0))
        inside_out[seq] = dot(mixed.astype(BF16), v_lin)
        k_out = k_left * jnp.where(second, 1.0, jnp.exp(end1))
        local_out[seq] = dot(k_out.astype(BF16), v_lin, TN)
        qr_out[seq] = (q_here * jnp.where(second, jnp.exp(end0), 1.0)).astype(BF16)
        decay_out[seq] = turned(jnp.exp(end0 + end1), HD)

    finish(0, x)

    f_right = remote(4, 1, 2, lo, to_right)
    f_left = remote(5, 3, 2, hi, to_left)
    relays = {
        "r0": remote(6, 1, 1, lo, partner),
        "l1": remote(7, 3, 3, hi, partner),
        "r1": remote(8, 1, 1, hi, partner),
        "l0": remote(9, 3, 3, lo, partner),
        "f0": remote(10, 2, 2, lo, partner),
        "f1": remote(11, 2, 2, hi, partner),
    }
    r0.wait_recv()
    f_right.start()
    l1.wait_recv()
    f_left.start()
    relays["r0"].start()
    relays["l1"].start()
    r1.wait_recv()
    relays["r1"].start()
    l0.wait_recv()
    relays["l0"].start()
    for c in small:
        c.wait_recv()
    relays["r0"].wait_recv()
    relays["r1"].wait_recv()
    finish(1, left)
    f_right.wait_recv()
    relays["f0"].start()
    f_left.wait_recv()
    relays["f1"].start()
    relays["l1"].wait_recv()
    relays["l0"].wait_recv()
    finish(3, right)
    relays["f0"].wait_recv()
    relays["f1"].wait_recv()
    finish(2, far)
    for c in (r0, l1, r1, l0, f_right, f_left, *relays.values(), *small):
        c.wait_send()


def mix_kernel(
    kv_ref,
    q_ref,
    qr_ref,
    inside_ref,
    local_ref,
    decay_ref,
    init_ref,
    lam_ref,
    mix_gain_ref,
    state_gain_ref,
    wa_hbm,
    wl_hbm,
    out_ref,
    wa,
    wl,
    kvbuf,
    qbuf,
    abuf,
    sin,
    sout,
    lbuf,
    fa,
    fl,
    w_sem,
    kv_send,
    kv_recv,
    q_send,
    q_recv,
    relay_send,
    a_send,
    a_recv,
    c_send,
    c_recv,
    l_send,
    l_recv,
    f_send,
    f_recv,
):
    x = lax.axis_index("fs")
    t = lax.axis_index("tp")
    z = lax.axis_index("sp")
    n_sp = lax.axis_size("sp")
    n_fs = lax.axis_size("fs")
    head = x * 2 + t
    odd = lax.rem(x, 2)
    pair = z // 2
    worker = lax.rem(z, 2) == odd
    w_seq = pair // 2
    w_tp = lax.rem(pair, 2)
    w_head = x * 2 + w_tp
    partner = {"tp": 1 - t}

    def plane(seq, xx, tt):
        return 2 * (2 * seq + tt) + lax.rem(xx, 2)

    load_a = pltpu.make_async_copy(wa_hbm, wa, w_sem.at[0])
    load_l = pltpu.make_async_copy(wl_hbm, wl, w_sem.at[1])
    load_a.start()
    load_l.start()

    barrier = pltpu.get_barrier_semaphore()

    def greet(dev, ok=None):
        def go():
            pl.semaphore_signal(barrier, inc=1, device_id=dev, device_id_type=MESH)

        if ok is None:
            go()
        else:
            pl.when(ok)(go)

    def greet_column(i, c):
        zz = lax.rem(z + i, n_sp)
        greet({"sp": zz})
        greet({"sp": zz, "tp": 1 - t})
        return c

    greet(partner)
    lax.fori_loop(1, n_sp, greet_column, 0)
    for i in range(1, n_fs):
        xx = lax.rem(x + i, n_fs)
        for tt in range(2):
            greet({"fs": xx, "tp": tt})
    for i in range(n_fs):
        xx = lax.rem(x + i, n_fs)
        for tt in range(2):
            pp = plane(x, xx, tt)
            greet({"fs": xx, "sp": pp}, None if i else pp != z)
    expected = 2 * n_sp - 1 + 2 * (n_fs - 1)
    is_worker = worker.astype(jnp.int32)
    expected = expected + is_worker * n_sp - is_worker * (w_seq == x).astype(jnp.int32)
    pl.semaphore_wait(barrier, expected)

    kv_core = lax.rem(z, 2)

    def kv_copy(seq, dst_z, dst_t):
        return pltpu.make_async_remote_copy(
            src_ref=kv_ref.at[seq],
            dst_ref=kvbuf.at[z],
            send_sem=kv_send.at[seq],
            recv_sem=kv_recv.at[z],
            device_id={"sp": dst_z, "tp": dst_t},
            device_id_type=MESH,
        )

    def q_copy(seq, dst_z, dst_t):
        return pltpu.make_async_remote_copy(
            src_ref=q_ref.at[seq, pl.ds(dst_t * HALF, HALF), :],
            dst_ref=qbuf.at[z],
            send_sem=q_send.at[seq, dst_t],
            recv_sem=q_recv.at[z],
            device_id={"sp": dst_z, "tp": dst_t},
            device_id_type=MESH,
        )

    def spread(start):
        for seq in range(4):
            pz = plane(seq, x, t)
            mine = (pz == z) & (kv_core == t)
            c = kv_copy(seq, pz, kv_core)
            pl.when(jnp.logical_not(mine))(c.start if start else c.wait_send)
            if start:

                @pl.when(mine)
                def _():
                    kvbuf[z] = kv_ref[seq]

            for tt in range(2):
                mine_q = (pz == z) & (t == tt)
                c = q_copy(seq, pz, tt)
                pl.when(jnp.logical_not(mine_q))(c.start if start else c.wait_send)
                if start:

                    @pl.when(mine_q)
                    def _():
                        qbuf[z] = q_ref[seq, tt * HALF : (tt + 1) * HALF, :]

    def chain_copy(seq):
        return pltpu.make_async_remote_copy(
            src_ref=sout.at[seq],
            dst_ref=sin.at[seq],
            send_sem=c_send.at[seq],
            recv_sem=c_recv.at[seq],
            device_id={"sp": lax.rem(z + 1, n_sp)},
            device_id_type=MESH,
        )

    def lin_copy(seq, tt):
        return pltpu.make_async_remote_copy(
            src_ref=lbuf.at[seq, pl.ds(tt * HALF, HALF), :],
            dst_ref=fl.at[tt, :, pl.ds(pl.multiple_of(head * HV, HV), HV)],
            send_sem=l_send.at[seq, tt],
            recv_sem=l_recv.at[head],
            device_id={"fs": seq, "tp": tt},
            device_id_type=MESH,
        )

    first, last = z == 0, z == n_sp - 1

    def chain():
        for seq in range(4):

            @pl.when(first)
            def _():
                sin[seq] = init_ref[seq].astype(BF16)
                d = decay_ref[seq]
                d = jnp.concatenate([d, d], axis=1)
                sout[seq] = (init_ref[seq] * d + local_ref[seq]).astype(BF16)
                chain_copy(seq).start()

            @pl.when(jnp.logical_not(first | last))
            def _():
                chain_copy(seq).wait_recv()
                d = decay_ref[seq]
                d = jnp.concatenate([d, d], axis=1)
                sout[seq] = (sin[seq].astype(F32) * d + local_ref[seq]).astype(BF16)
                chain_copy(seq).start()

        for seq in range(4):

            @pl.when(last)
            def _():
                chain_copy(seq).wait_recv()

            raw = inside_ref[seq] + dot(qr_ref[seq], sin[seq])
            mean = jnp.mean(raw * raw, axis=1, keepdims=True)
            lin = (raw * lax.rsqrt(mean + EPS) * state_gain_ref[...]).astype(BF16)
            lbuf[seq] = lin
            for tt in range(2):
                mine = (x == seq) & (t == tt)
                pl.when(jnp.logical_not(mine))(lin_copy(seq, tt).start)

                @pl.when(mine)
                def _():
                    fl[tt, :, pl.ds(pl.multiple_of(head * HV, HV), HV)] = lin[
                        tt * HALF : (tt + 1) * HALF
                    ]

    def relay_copy(j):
        zz = t + 2 * j
        return pltpu.make_async_remote_copy(
            src_ref=kvbuf.at[zz],
            dst_ref=kvbuf.at[zz],
            send_sem=relay_send.at[j],
            recv_sem=kv_recv.at[zz],
            device_id=partner,
            device_id_type=MESH,
        )

    def kv_arrival(zz):
        return pltpu.make_async_remote_copy(
            src_ref=kv_ref.at[0],
            dst_ref=kvbuf.at[zz],
            send_sem=kv_send.at[0],
            recv_sem=kv_recv.at[zz],
            device_id=partner,
            device_id_type=MESH,
        )

    def q_arrival(zz):
        return pltpu.make_async_remote_copy(
            src_ref=q_ref.at[0, pl.ds(0, HALF), :],
            dst_ref=qbuf.at[zz],
            send_sem=q_send.at[0, 0],
            recv_sem=q_recv.at[zz],
            device_id=partner,
            device_id_type=MESH,
        )

    def a_copy(i):
        return pltpu.make_async_remote_copy(
            src_ref=abuf.at[i],
            dst_ref=fa.at[t, :, pl.ds(pl.multiple_of(w_head * HD, HD), HD)],
            send_sem=a_send.at[i],
            recv_sem=a_recv.at[w_head],
            device_id={"fs": w_seq, "sp": i},
            device_id_type=MESH,
        )

    def attend():
        lam = lam_ref[w_head]
        own = t == w_tp
        for g in range(4):
            span = 512 * (g + 1)
            for j in range(2 * g, 2 * g + 2):
                zz = t + 2 * j
                pl.when(jnp.logical_not(own & (zz == z)))(kv_arrival(zz).wait_recv)
                relay_copy(j).start()
            for i in range(4 * g, 4 * g + 4):
                pl.when(jnp.logical_not(own & (z == i)))(q_arrival(i).wait_recv)
            for j in range(2 * g, 2 * g + 2):
                kv_arrival((1 - t) + 2 * j).wait_recv()

            def one(i, c):
                qi = qbuf[i]
                lane = iota((HALF, HD), 1)
                zero = jnp.zeros_like(qi)
                q2 = jnp.concatenate(
                    [jnp.where(lane < HALF, qi, zero), jnp.where(lane < HALF, zero, qi)], axis=0
                )
                n_old = 4 * g
                keys = kvbuf[n_old : n_old + 4, :, 0:HD].reshape(512, HD)
                vals = kvbuf[n_old : n_old + 4, :, HD:].reshape(512, HD)
                s = dot(q2, keys, NT)
                limit = (2 * i + t + 1) * BLK - span + 512
                s = jnp.where(iota(s.shape, 1) < limit, s, -jnp.inf)
                top = jnp.max(s, axis=1, keepdims=True)
                if g:
                    old_keys = kvbuf[0:n_old, :, 0:HD].reshape(span - 512, HD)
                    old_vals = kvbuf[0:n_old, :, HD:].reshape(span - 512, HD)
                    s_old = dot(q2, old_keys, NT)
                    top = jnp.maximum(top, jnp.max(s_old, axis=1, keepdims=True))
                p = jnp.exp(s - top)
                total = jnp.sum(p, axis=1, keepdims=True)
                acc = dot(p.astype(BF16), vals)
                if g:
                    p_old = jnp.exp(s_old - top)
                    total = total + jnp.sum(p_old, axis=1, keepdims=True)
                    acc = acc + dot(p_old.astype(BF16), old_vals)
                acc = acc / total
                diff = acc[:HALF] - lam * acc[HALF:]
                mean = jnp.mean(diff * diff, axis=1, keepdims=True)
                res = (diff * lax.rsqrt(mean + EPS) * mix_gain_ref[...]).astype(BF16)
                abuf[i] = res
                mine = (x == w_seq) & (z == i)
                pl.when(jnp.logical_not(mine))(a_copy(i).start)

                @pl.when(mine)
                def _():
                    fa[t, :, pl.ds(pl.multiple_of(w_head * HD, HD), HD)] = res

                return c

            lax.fori_loop(4 * g, 4 * g + 4, one, 0)

    spread(True)

    early = (z <= CHAIN_FIRST_UP_TO).astype(jnp.int32)

    def phase(i, c):
        is_chain = lax.rem(i + early, 2) == 1
        pl.when(is_chain)(chain)
        pl.when(jnp.logical_not(is_chain) & worker)(attend)
        return c

    lax.fori_loop(0, 2, phase, 0)

    def a_arrival(hh):
        return pltpu.make_async_remote_copy(
            src_ref=abuf.at[0],
            dst_ref=fa.at[t, :, pl.ds(hh * HD, HD)],
            send_sem=a_send.at[0],
            recv_sem=a_recv.at[hh],
            device_id=partner,
            device_id_type=MESH,
        )

    def l_arrival(hh):
        return pltpu.make_async_remote_copy(
            src_ref=lbuf.at[0, pl.ds(0, HALF), :],
            dst_ref=fl.at[t, :, pl.ds(hh * HV, HV)],
            send_sem=l_send.at[0, 0],
            recv_sem=l_recv.at[hh],
            device_id=partner,
            device_id_type=MESH,
        )

    def swap(buf, i):
        return pltpu.make_async_remote_copy(
            src_ref=buf.at[t],
            dst_ref=buf.at[t],
            send_sem=f_send.at[i],
            recv_sem=f_recv.at[i],
            device_id=partner,
            device_id_type=MESH,
        )

    for hh in range(HEADS):
        from_me = (x == hh // 2) & (z == plane(x, hh // 2, hh % 2))
        pl.when(jnp.logical_not(from_me))(a_arrival(hh).wait_recv)
    swap(fa, 0).start()
    load_a.wait()
    load_l.wait()
    swap(fa, 0).wait_recv()
    acc = dot(fa[...].reshape(2 * HALF, HEADS * HD), wa[...])
    for hh in range(HEADS):
        pl.when(head != hh)(l_arrival(hh).wait_recv)
    swap(fl, 1).start()
    swap(fl, 1).wait_recv()
    acc = acc + dot(fl[...].reshape(2 * HALF, HEADS * HV), wl[...])
    out_ref[...] = acc.astype(BF16)

    swap(fa, 0).wait_send()
    swap(fl, 1).wait_send()
    spread(False)
    for seq in range(4):
        pl.when(jnp.logical_not(last))(chain_copy(seq).wait_send)
        for tt in range(2):
            mine = (x == seq) & (t == tt)
            pl.when(jnp.logical_not(mine))(lin_copy(seq, tt).wait_send)

    @pl.when(worker)
    def _():
        for j in range(8):
            relay_copy(j).wait_send()

        def done(i, c):
            mine = (x == w_seq) & (z == i)
            pl.when(jnp.logical_not(mine))(a_copy(i).wait_send)
            return c

        lax.fori_loop(0, n_sp, done, 0)


def body(
    tokens,
    norm_gain,
    query_attend,
    key_attend,
    value_attend,
    query_linear,
    key_linear,
    value_linear,
    decay_down,
    decay_up,
    decay_bias,
    log_retain,
    query_gain,
    key_gain,
    diff_lambda,
    mix_gain,
    state_gain,
    init_state,
    output_attend,
    output_linear,
):
    rows, width = tokens.shape[1:]
    n_fs = lax.axis_size("fs")
    n_sp = lax.axis_size("sp")
    cols = output_attend.shape[1]
    flat = [
        w.reshape(w.shape[0], -1)
        for w in (query_attend, key_attend, value_attend, query_linear, key_linear, value_linear)
    ]
    total = sum(w.shape[1] for w in flat)
    vmem = pl.BlockSpec(memory_space=pltpu.VMEM)
    smem = pl.BlockSpec(memory_space=pltpu.SMEM)
    hbm = pl.BlockSpec(memory_space=pl.ANY)
    dma = pltpu.SemaphoreType.DMA

    made = pl.pallas_call(
        project_kernel,
        out_shape=[
            jax.ShapeDtypeStruct((n_fs, rows, 2 * HD), BF16),
            jax.ShapeDtypeStruct((n_fs, rows, HD), BF16),
            jax.ShapeDtypeStruct((n_fs, rows, HD), BF16),
            jax.ShapeDtypeStruct((n_fs, rows, HV), F32),
            jax.ShapeDtypeStruct((n_fs, HD, HV), F32),
            jax.ShapeDtypeStruct((n_fs, HD, HD), F32),
        ],
        in_specs=[vmem, vmem] + [hbm] * 6 + [vmem] * 6,
        out_specs=[vmem] * 6,
        scratch_shapes=[
            pltpu.VMEM((width, total), BF16),
            pltpu.VMEM((n_fs, rows, width), BF16),
            pltpu.VMEM((n_fs, HEADS, rows), F32),
            dma((6,)),
            dma((12,)),
            dma((12,)),
            dma((3,)),
            dma((3,)),
        ],
        compiler_params=pltpu.CompilerParams(
            collective_id=0, has_side_effects=True, vmem_limit_bytes=40 * 1024 * 1024
        ),
        name="project",
    )(
        tokens[0],
        norm_gain.reshape(1, -1),
        *flat,
        decay_down.T,
        decay_up.reshape(-1, HD),
        decay_bias,
        log_retain[0].T,
        query_gain.reshape(1, -1),
        key_gain,
    )

    out = pl.pallas_call(
        mix_kernel,
        out_shape=jax.ShapeDtypeStruct((rows, cols), BF16),
        in_specs=[vmem] * 6 + [vmem, smem, vmem, vmem, hbm, hbm],
        out_specs=vmem,
        scratch_shapes=[
            pltpu.VMEM(output_attend.shape, BF16),
            pltpu.VMEM(output_linear.shape, BF16),
            pltpu.VMEM((n_sp, rows, 2 * HD), BF16),
            pltpu.VMEM((n_sp, HALF, HD), BF16),
            pltpu.VMEM((n_sp, HALF, HD), BF16),
            pltpu.VMEM((n_fs, HD, HV), BF16),
            pltpu.VMEM((n_fs, HD, HV), BF16),
            pltpu.VMEM((n_fs, rows, HV), BF16),
            pltpu.VMEM((2, HALF, HEADS * HD), BF16),
            pltpu.VMEM((2, HALF, HEADS * HV), BF16),
            dma((2,)),
            dma((4,)),
            dma((n_sp,)),
            dma((4, 2)),
            dma((n_sp,)),
            dma((8,)),
            dma((n_sp,)),
            dma((HEADS,)),
            dma((4,)),
            dma((4,)),
            dma((4, 2)),
            dma((HEADS,)),
            dma((2,)),
            dma((2,)),
        ],
        compiler_params=pltpu.CompilerParams(
            collective_id=1, has_side_effects=True, vmem_limit_bytes=40 * 1024 * 1024
        ),
        name="mix",
    )(
        *made,
        init_state.reshape(n_fs, HD, HV),
        diff_lambda,
        mix_gain.reshape(1, -1),
        state_gain.reshape(1, -1),
        output_attend,
        output_linear,
    )
    return out[None]


def solution(mesh):
    heads = P(None, ("fs", "tp"), None)
    in_specs = (
        P(("grp", "fs"), "sp", None),
        P(),
        heads,
        heads,
        heads,
        heads,
        heads,
        heads,
        P(),
        P(),
        P(),
        P(("grp", "fs"), "sp", None),
        P(),
        P(),
        P(),
        P(),
        P(),
        P("grp", ("fs", "tp"), None, None),
        P(None, "tp"),
        P(None, "tp"),
    )
    out_specs = P(("grp", "fs"), "sp", "tp")
    return jax.shard_map(body, mesh=mesh, in_specs=in_specs, out_specs=out_specs, check_vma=False)
```

```python
import functools

import jax
import jax.numpy as jnp
from jax import lax
from jax.experimental import pallas as pl
from jax.experimental.pallas import tpu as pltpu
from jax.sharding import PartitionSpec as P

HEADS = 8
HALF = 64
HD = 128
HV = 256
BLK = 64
RANK = 32
EPS = 1e-06
TAU = 16.0
MESH = pl.DeviceIdType.MESH
F32 = jnp.float32
BF16 = jnp.bfloat16
NT = (((1,), (1,)), ((), ()))
TN = (((0,), (0,)), ((), ()))


def dot(a, b, dims=(((1,), (0,)), ((), ())), **kw):
    return lax.dot_general(a, b, dims, preferred_element_type=F32, **kw)


def iota(shape, dim):
    return lax.broadcasted_iota(jnp.int32, shape, dim)


def turned(row, n):
    return jnp.transpose(jnp.broadcast_to(row, (n, row.shape[-1])))


def unit_norm(x, gain):
    left = iota(x.shape, 1) < HALF
    sq = x * x
    a = jnp.sum(jnp.where(left, sq, 0.0), axis=1, keepdims=True)
    b = jnp.sum(jnp.where(left, 0.0, sq), axis=1, keepdims=True)
    mean = jnp.where(left, a, b) * (1.0 / HALF)
    return (x * lax.rsqrt(mean + EPS) * gain).astype(BF16)


def layer_kernel(
    tok_hbm,
    gain_hbm,
    wqa,
    wka,
    wva,
    wql,
    wkl,
    wvl,
    down_hbm,
    up_hbm,
    bias_hbm,
    retain_hbm,
    qgain_hbm,
    kgain_hbm,
    lam_ref,
    mix_gain_hbm,
    state_gain_hbm,
    init_hbm,
    wa_hbm,
    wl_hbm,
    out_ref,
    tok,
    gain_v,
    weights,
    down,
    up,
    bias_v,
    qgain_v,
    kgain_v,
    mix_gain,
    state_gain,
    init,
    wa,
    wl,
    gath,
    rets,
    kvs,
    qs,
    qr,
    inside,
    local,
    dec,
    kvbuf,
    qbuf,
    abuf,
    sin,
    sout,
    lbuf,
    fa,
    fl,
    in_sem,
    send,
    recv,
    r_send,
    r_recv,
    kv_send,
    kv_recv,
    q_send,
    q_recv,
    relay_send,
    a_send,
    a_recv,
    c_send,
    c_recv,
    l_send,
    l_recv,
    f_send,
    f_recv,
    up_sem,
    ready_sem,
):
    x = lax.axis_index("fs")
    t = lax.axis_index("tp")
    z = lax.axis_index("sp")
    n_sp = lax.axis_size("sp")
    n_fs = lax.axis_size("fs")
    n_work = 2 * n_fs
    right, left, far = lax.rem(x + 1, n_fs), lax.rem(x + n_fs - 1, n_fs), lax.rem(x + 2, n_fs)
    seqs = (x, left, far, right)
    order = (0, 1, 3, 2)
    head = x * 2 + t
    rows = tok.shape[0]
    partner = {"tp": 1 - t}
    first, last = z == 0, z == n_sp - 1
    worker = z < n_work
    w_seq = z // 2
    w_tp = lax.rem(z, 2)
    w_head = x * 2 + w_tp
    kv_core = lax.rem(z, 2)

    barrier = pltpu.get_barrier_semaphore()

    def tell(sem, dev):
        pl.semaphore_signal(sem, inc=1, device_id=dev, device_id_type=MESH)

    for peer in (right, left, far):
        for tt in range(2):
            tell(barrier, {"fs": peer, "tp": tt})
    tell(barrier, partner)
    pl.when(jnp.logical_not(first))(lambda: tell(barrier, {"sp": lax.rem(z + n_sp - 1, n_sp)}))
    pl.when(jnp.logical_not(last))(lambda: tell(barrier, {"sp": lax.rem(z + 1, n_sp)}))

    loads = []

    def load(src, dst):
        c = pltpu.make_async_copy(src, dst, in_sem.at[len(loads)])
        loads.append(c)
        c.start()

    load(tok_hbm, tok)
    load(gain_hbm, gain_v)
    load(retain_hbm, rets.at[0])
    at = 0
    for w in (wqa, wka, wva, wql, wkl, wvl):
        width = w.shape[1]
        load(w, weights.at[:, pl.ds(at, width)])
        at += width
    load(down_hbm, down)
    load(up_hbm, up)
    load(bias_hbm, bias_v)
    load(qgain_hbm, qgain_v)
    load(kgain_hbm, kgain_v)
    load(mix_gain_hbm, mix_gain)
    load(state_gain_hbm, state_gain)
    for slot in range(n_fs):
        load(init_hbm.at[seqs[slot]], init.at[slot])
    load(wa_hbm, wa)
    load(wl_hbm, wl)
    for c in loads[:3]:
        c.wait()
    gain = gain_v[...]

    def normalize(start):
        part = tok[pl.ds(start, 32), :].astype(F32)
        mean = jnp.mean(part * part, axis=1, keepdims=True)
        gath[0, pl.ds(start, 32), :] = (part * lax.rsqrt(mean + EPS) * gain).astype(BF16)

    lo = pl.multiple_of(t * 64, 64)
    hi = pl.multiple_of(t * 64 + 32, 32)
    other = pl.multiple_of((1 - t) * 64, 64)
    other_hi = pl.multiple_of((1 - t) * 64 + 32, 32)
    normalize(lo)
    normalize(hi)
    with jax.named_scope("bar"):
        pl.semaphore_wait(
            barrier,
            7 + jnp.logical_not(first).astype(jnp.int32) + jnp.logical_not(last).astype(jnp.int32),
        )

    def remote(i, slot_from, slot_to, start, peer):
        return pltpu.make_async_remote_copy(
            src_ref=gath.at[slot_from, pl.ds(start, 32), :],
            dst_ref=gath.at[slot_to, pl.ds(start, 32), :],
            send_sem=send.at[i],
            recv_sem=recv.at[i],
            device_id=peer,
            device_id_type=MESH,
        )

    to_right = {"fs": right}
    to_left = {"fs": left}
    r0 = remote(0, 0, 1, lo, to_right)
    l1 = remote(1, 0, 3, hi, to_left)
    r1 = remote(2, 0, 1, hi, to_right)
    l0 = remote(3, 0, 3, lo, to_left)
    for c in (r0, l1, r1, l0):
        c.start()
    small = []
    for i, (slot, peer) in enumerate(((1, right), (3, left), (2, far))):
        small.append(
            pltpu.make_async_remote_copy(
                src_ref=rets.at[0],
                dst_ref=rets.at[slot],
                send_sem=r_send.at[i],
                recv_sem=r_recv.at[i],
                device_id={"fs": peer},
                device_id_type=MESH,
            )
        )
    for c in small:
        c.start()

    with jax.named_scope("upw"):

        @pl.when(jnp.logical_not(first))
        def _():
            pl.semaphore_wait(up_sem, 1)

    pl.when(jnp.logical_not(last))(lambda: tell(up_sem, {"sp": lax.rem(z + 1, n_sp)}))

    @pl.when(worker)
    def _():
        def lower(zz, c):
            tell(ready_sem, {"sp": zz, "tp": 0})
            tell(ready_sem, {"sp": zz, "tp": 1})
            return c

        lax.fori_loop(0, z, lower, 0)

    normalize(other)
    normalize(other_hi)
    with jax.named_scope("wwait"):
        for c in loads[3:14]:
            c.wait()

    up_rows = up[...]
    pick = iota((RANK, RANK * HEADS), 1) == iota((RANK, RANK * HEADS), 0) * HEADS + head
    pick = jnp.where(pick, 1.0, 0.0).astype(BF16)
    bias = bias_v[pl.ds(head, 1), :]
    qg = qgain_v[...]
    qgain = jnp.concatenate([qg, qg], axis=1)
    kg = kgain_v[pl.ds(head, 1)][0]
    kgain = jnp.concatenate([kg[0:1], kg[1:2]], axis=1)
    rr, cc = iota((rows, rows), 0), iota((rows, rows), 1)
    same = (rr // BLK) == (cc // BLK)
    tri = jnp.where(same & (rr >= cc), 1.0, 0.0)
    second = iota((rows, HD), 0) >= BLK

    def finish(slot):
        act = gath[slot]
        got = dot(act, weights[...]).astype(BF16)
        low = dot(act, down[...], NT).astype(BF16)
        pre = dot(dot(low, pick).astype(BF16), up_rows) + bias
        log_sig = jnp.minimum(pre, 0.0) - jnp.log1p(jnp.exp(-jnp.abs(pre)))
        keep = jnp.sum(
            jnp.where(iota((HEADS, rows), 0) == head, rets[slot], 0.0), axis=0, keepdims=True
        )
        log_decay = log_sig * (1.0 / TAU) + turned(keep, HD)
        run = dot(tri, log_decay, precision=lax.Precision.HIGHEST)
        q_unit = unit_norm(got[:, 0:HD].astype(F32), qgain)
        k_unit = unit_norm(got[:, HD : 2 * HD].astype(F32), kgain)
        kvs[slot, :, 0:HD] = k_unit
        kvs[slot, :, HD : 2 * HD] = got[:, 2 * HD : 3 * HD]
        qs[slot] = (q_unit.astype(F32) * (HALF**-0.5)).astype(BF16)
        q_lin = got[:, 3 * HD : 4 * HD].astype(F32) * (HD**-0.5)
        k_lin = got[:, 4 * HD : 5 * HD].astype(F32)
        v_lin = got[:, 5 * HD :]
        mid = BLK // 2
        pivot = jnp.where(second, run[BLK + mid : BLK + mid + 1], run[mid : mid + 1])
        end0, end1 = run[BLK - 1 : BLK], run[2 * BLK - 1 : 2 * BLK]
        ends = jnp.where(second, end1, end0)
        scores = dot(
            (q_lin * jnp.exp(run - pivot)).astype(BF16),
            (k_lin * jnp.exp(pivot - run)).astype(BF16),
            NT,
        )
        q_here = q_lin * jnp.exp(run)
        k_left = k_lin * jnp.exp(ends - run)
        across = dot(q_here.astype(BF16), k_left.astype(BF16), NT)
        later = (rr >= BLK) & (cc < BLK)
        mixed = jnp.where(same & (rr >= cc), scores, jnp.where(later, across, 0.0))
        inside[slot] = dot(mixed.astype(BF16), v_lin)
        k_out = k_left * jnp.where(second, 1.0, jnp.exp(end1))
        local[slot] = dot(k_out.astype(BF16), v_lin, TN)
        qr[slot] = (q_here * jnp.where(second, jnp.exp(end0), 1.0)).astype(BF16)
        dec[slot] = turned(jnp.exp(end0 + end1), HD)

    finish(0)

    f_right = remote(4, 1, 2, lo, to_right)
    f_left = remote(5, 3, 2, hi, to_left)
    relays = {
        "r0": remote(6, 1, 1, lo, partner),
        "l1": remote(7, 3, 3, hi, partner),
        "r1": remote(8, 1, 1, hi, partner),
        "l0": remote(9, 3, 3, lo, partner),
        "f0": remote(10, 2, 2, lo, partner),
        "f1": remote(11, 2, 2, hi, partner),
    }
    with jax.named_scope("p_r0"):
        r0.wait_recv()
    f_right.start()
    relays["r0"].start()
    l1.wait_recv()
    f_left.start()
    relays["l1"].start()
    with jax.named_scope("p_r1"):
        r1.wait_recv()
    relays["r1"].start()
    l0.wait_recv()
    relays["l0"].start()
    for c in small:
        c.wait_recv()
    with jax.named_scope("p_rel1"):
        relays["r0"].wait_recv()
        relays["r1"].wait_recv()
    finish(1)
    with jax.named_scope("p_f"):
        f_right.wait_recv()
        relays["f0"].start()
        f_left.wait_recv()
        relays["f1"].start()
        relays["l1"].wait_recv()
        relays["l0"].wait_recv()
    finish(3)
    with jax.named_scope("p_relf"):
        relays["f0"].wait_recv()
        relays["f1"].wait_recv()
    finish(2)

    def kv_copy(slot, dst_z):
        return pltpu.make_async_remote_copy(
            src_ref=kvs.at[slot],
            dst_ref=kvbuf.at[z],
            send_sem=kv_send.at[slot],
            recv_sem=kv_recv.at[z],
            device_id={"sp": dst_z, "tp": kv_core},
            device_id_type=MESH,
        )

    def q_copy(slot, dst_z, dst_t):
        return pltpu.make_async_remote_copy(
            src_ref=qs.at[slot, pl.ds(dst_t * HALF, HALF), :],
            dst_ref=qbuf.at[z],
            send_sem=q_send.at[slot, dst_t],
            recv_sem=q_recv.at[z],
            device_id={"sp": dst_z, "tp": dst_t},
            device_id_type=MESH,
        )

    def spread(start):
        for slot in order:
            pz = 2 * seqs[slot] + t
            mine = (pz == z) & (kv_core == t)
            c = kv_copy(slot, pz)
            pl.when(jnp.logical_not(mine))(c.start if start else c.wait_send)
            if start:

                @pl.when(mine)
                def _():
                    kvbuf[z] = kvs[slot]

            for tt in range(2):
                mine_q = (pz == z) & (t == tt)
                c = q_copy(slot, pz, tt)
                pl.when(jnp.logical_not(mine_q))(c.start if start else c.wait_send)
                if start:

                    @pl.when(mine_q)
                    def _():
                        qbuf[z] = qs[slot, tt * HALF : (tt + 1) * HALF, :]

    n_piece = 2
    piece = HD // n_piece

    def chain_copy(slot, k):
        part = pl.ds(k * piece, piece)
        return pltpu.make_async_remote_copy(
            src_ref=sout.at[slot, part, :],
            dst_ref=sin.at[slot, part, :],
            send_sem=c_send.at[slot, k],
            recv_sem=c_recv.at[slot, k],
            device_id={"sp": lax.rem(z + 1, n_sp)},
            device_id_type=MESH,
        )

    def lin_copy(slot, tt):
        return pltpu.make_async_remote_copy(
            src_ref=lbuf.at[slot, pl.ds(tt * HALF, HALF), :],
            dst_ref=fl.at[tt, :, pl.ds(pl.multiple_of(head * HV, HV), HV)],
            send_sem=l_send.at[slot, tt],
            recv_sem=l_recv.at[head],
            device_id={"fs": seqs[slot], "tp": tt},
            device_id_type=MESH,
        )

    def passed_on(slot, k, value):
        part = slice(k * piece, (k + 1) * piece)
        d = dec[slot, part, :]
        d = jnp.concatenate([d, d], axis=1)
        sout[slot, part, :] = (value * d + local[slot, part, :]).astype(BF16)
        chain_copy(slot, k).start()

    def chain_start():
        for c in loads[16:20]:
            c.wait()
        for slot in order:
            sin[slot] = init[slot].astype(BF16)
            for k in range(n_piece):
                passed_on(slot, k, init[slot, k * piece : (k + 1) * piece, :])

    def chain():
        @pl.when(jnp.logical_not(first | last))
        def _():
            for slot in order:
                for k in range(n_piece):
                    with jax.named_scope("cwait"):
                        chain_copy(slot, k).wait_recv()
                    passed_on(slot, k, sin[slot, k * piece : (k + 1) * piece, :].astype(F32))

        for slot in order:

            @pl.when(last)
            def _():
                with jax.named_scope("cwait"):
                    for k in range(n_piece):
                        chain_copy(slot, k).wait_recv()

            raw = inside[slot] + dot(qr[slot], sin[slot])
            mean = jnp.mean(raw * raw, axis=1, keepdims=True)
            lin = (raw * lax.rsqrt(mean + EPS) * state_gain[...]).astype(BF16)
            lbuf[slot] = lin
            for tt in range(2):
                if slot:
                    lin_copy(slot, tt).start()
                else:
                    pl.when(t != tt)(lin_copy(slot, tt).start)

                    @pl.when(t == tt)
                    def _():
                        fl[tt, :, pl.ds(pl.multiple_of(head * HV, HV), HV)] = lin[
                            tt * HALF : (tt + 1) * HALF
                        ]

    def relay_copy(j):
        zz = t + 2 * j
        return pltpu.make_async_remote_copy(
            src_ref=kvbuf.at[zz],
            dst_ref=kvbuf.at[zz],
            send_sem=relay_send.at[j],
            recv_sem=kv_recv.at[zz],
            device_id=partner,
            device_id_type=MESH,
        )

    def kv_arrival(zz):
        return pltpu.make_async_remote_copy(
            src_ref=kvs.at[0],
            dst_ref=kvbuf.at[zz],
            send_sem=kv_send.at[0],
            recv_sem=kv_recv.at[zz],
            device_id=partner,
            device_id_type=MESH,
        )

    def q_arrival(zz):
        return pltpu.make_async_remote_copy(
            src_ref=qs.at[0, pl.ds(0, HALF), :],
            dst_ref=qbuf.at[zz],
            send_sem=q_send.at[0, 0],
            recv_sem=q_recv.at[zz],
            device_id=partner,
            device_id_type=MESH,
        )

    def a_copy(i):
        return pltpu.make_async_remote_copy(
            src_ref=abuf.at[i],
            dst_ref=fa.at[t, :, pl.ds(pl.multiple_of(w_head * HD, HD), HD)],
            send_sem=a_send.at[i],
            recv_sem=a_recv.at[w_head],
            device_id={"fs": w_seq, "sp": i},
            device_id_type=MESH,
        )

    def attend(g):
        lam = lam_ref[w_head]
        own = t == w_tp
        span = 512 * (g + 1)
        with jax.named_scope("kvwait"):
            for j in range(2 * g, 2 * g + 2):
                zz = t + 2 * j
                pl.when(jnp.logical_not(own & (zz == z)))(kv_arrival(zz).wait_recv)
                relay_copy(j).start()
        with jax.named_scope("qwait"):
            for i in range(4 * g, 4 * g + 4):
                pl.when(jnp.logical_not(own & (z == i)))(q_arrival(i).wait_recv)
        with jax.named_scope("rwait"):
            for j in range(2 * g, 2 * g + 2):
                kv_arrival((1 - t) + 2 * j).wait_recv()

        def one(i, c):
            qi = qbuf[i]
            lane = iota((HALF, HD), 1)
            zero = jnp.zeros_like(qi)
            q2 = jnp.concatenate(
                [jnp.where(lane < HALF, qi, zero), jnp.where(lane < HALF, zero, qi)], axis=0
            )
            n_old = 4 * g
            keys = kvbuf[n_old : n_old + 4, :, 0:HD].reshape(512, HD)
            vals = kvbuf[n_old : n_old + 4, :, HD:].reshape(512, HD)
            s = dot(q2, keys, NT)
            limit = (2 * i + t + 1) * BLK - span + 512
            s = jnp.where(iota(s.shape, 1) < limit, s, -jnp.inf)
            top = jnp.max(s, axis=1, keepdims=True)
            if g:
                old_keys = kvbuf[0:n_old, :, 0:HD].reshape(span - 512, HD)
                old_vals = kvbuf[0:n_old, :, HD:].reshape(span - 512, HD)
                s_old = dot(q2, old_keys, NT)
                top = jnp.maximum(top, jnp.max(s_old, axis=1, keepdims=True))
            p = jnp.exp(s - top)
            total = jnp.sum(p, axis=1, keepdims=True)
            acc = dot(p.astype(BF16), vals)
            if g:
                p_old = jnp.exp(s_old - top)
                total = total + jnp.sum(p_old, axis=1, keepdims=True)
                acc = acc + dot(p_old.astype(BF16), old_vals)
            acc = acc / total
            diff = acc[:HALF] - lam * acc[HALF:]
            mean = jnp.mean(diff * diff, axis=1, keepdims=True)
            res = (diff * lax.rsqrt(mean + EPS) * mix_gain[...]).astype(BF16)
            abuf[i] = res
            mine = (x == w_seq) & (z == i)
            pl.when(jnp.logical_not(mine))(a_copy(i).start)

            @pl.when(mine)
            def _():
                fa[t, :, pl.ds(pl.multiple_of(w_head * HD, HD), HD)] = res

            return c

        with jax.named_scope("attn"):
            lax.fori_loop(4 * g, 4 * g + 4, one, 0)

    for c in loads[14:16]:
        c.wait()
    pl.when(first)(chain_start)
    above = jnp.maximum(n_work - 1 - z, 0)
    with jax.named_scope("ready"):

        @pl.when(above > 0)
        def _():
            pl.semaphore_wait(ready_sem, 2 * above)

    with jax.named_scope("spread"):
        spread(True)

    chain_at = jnp.where(z < 4, 0, 1)

    def step(i, c):
        pl.when(i == chain_at)(chain)
        for g in range(4):
            pl.when(worker & (i == g))(functools.partial(attend, g))
        return c

    lax.fori_loop(0, 4, step, 0)

    @pl.when(jnp.logical_not(first))
    def _():
        for c in loads[16:20]:
            c.wait()

    def a_arrival(hh):
        return pltpu.make_async_remote_copy(
            src_ref=abuf.at[0],
            dst_ref=fa.at[t, :, pl.ds(hh * HD, HD)],
            send_sem=a_send.at[0],
            recv_sem=a_recv.at[hh],
            device_id=partner,
            device_id_type=MESH,
        )

    def l_arrival(hh):
        return pltpu.make_async_remote_copy(
            src_ref=lbuf.at[0, pl.ds(0, HALF), :],
            dst_ref=fl.at[t, :, pl.ds(hh * HV, HV)],
            send_sem=l_send.at[0, 0],
            recv_sem=l_recv.at[hh],
            device_id=partner,
            device_id_type=MESH,
        )

    def swap(buf, i):
        return pltpu.make_async_remote_copy(
            src_ref=buf.at[t],
            dst_ref=buf.at[t],
            send_sem=f_send.at[i],
            recv_sem=f_recv.at[i],
            device_id=partner,
            device_id_type=MESH,
        )

    for c in loads[20:]:
        c.wait()
    with jax.named_scope("await"):
        for hh in range(HEADS):
            from_me = (x == hh // 2) & (z == 2 * x + hh % 2)
            pl.when(jnp.logical_not(from_me))(a_arrival(hh).wait_recv)
    swap(fa, 0).start()
    with jax.named_scope("lwait"):
        for hh in range(HEADS):
            pl.when(head != hh)(l_arrival(hh).wait_recv)
    swap(fl, 1).start()
    swap(fa, 0).wait_recv()
    acc = dot(fa[...].reshape(2 * HALF, HEADS * HD), wa[...])
    with jax.named_scope("lswap"):
        swap(fl, 1).wait_recv()
    acc = acc + dot(fl[...].reshape(2 * HALF, HEADS * HV), wl[...])
    out_ref[...] = acc.astype(BF16)

    with jax.named_scope("drain"):
        swap(fa, 0).wait_send()
        swap(fl, 1).wait_send()
        for c in (r0, l1, r1, l0, f_right, f_left, *relays.values(), *small):
            c.wait_send()
        spread(False)
        for slot in order:
            for k in range(n_piece):
                pl.when(jnp.logical_not(last))(chain_copy(slot, k).wait_send)
            for tt in range(2):
                if slot:
                    lin_copy(slot, tt).wait_send()
                else:
                    pl.when(t != tt)(lin_copy(slot, tt).wait_send)

        @pl.when(worker)
        def _():
            for j in range(n_sp // 2):
                relay_copy(j).wait_send()

            def done(i, c):
                mine = (x == w_seq) & (z == i)
                pl.when(jnp.logical_not(mine))(a_copy(i).wait_send)
                return c

            lax.fori_loop(0, n_sp, done, 0)


def body(
    tokens,
    norm_gain,
    query_attend,
    key_attend,
    value_attend,
    query_linear,
    key_linear,
    value_linear,
    decay_down,
    decay_up,
    decay_bias,
    log_retain,
    query_gain,
    key_gain,
    diff_lambda,
    mix_gain,
    state_gain,
    init_state,
    output_attend,
    output_linear,
):
    rows, width = tokens.shape[1:]
    n_fs = lax.axis_size("fs")
    n_sp = lax.axis_size("sp")
    cols = output_attend.shape[1]
    flat = [
        w.reshape(w.shape[0], -1)
        for w in (query_attend, key_attend, value_attend, query_linear, key_linear, value_linear)
    ]
    total = sum(w.shape[1] for w in flat)
    vmem = pl.BlockSpec(memory_space=pltpu.VMEM)
    smem = pl.BlockSpec(memory_space=pltpu.SMEM)
    hbm = pl.BlockSpec(memory_space=pl.ANY)
    dma = pltpu.SemaphoreType.DMA
    V = pltpu.VMEM

    out = pl.pallas_call(
        layer_kernel,
        out_shape=jax.ShapeDtypeStruct((rows, cols), BF16),
        in_specs=[hbm] * 14 + [smem] + [hbm] * 5,
        out_specs=vmem,
        scratch_shapes=[
            V((rows, width), BF16),
            V((1, width), F32),
            V((width, total), BF16),
            V((RANK, width), BF16),
            V((RANK * HEADS, HD), BF16),
            V((HEADS, HD), F32),
            V((1, HALF), F32),
            V((HEADS, 2, HALF), F32),
            V((1, HD), F32),
            V((1, HV), F32),
            V((n_fs, HD, HV), F32),
            V(output_attend.shape, BF16),
            V(output_linear.shape, BF16),
            V((n_fs, rows, width), BF16),
            V((n_fs, HEADS, rows), F32),
            V((n_fs, rows, 2 * HD), BF16),
            V((n_fs, rows, HD), BF16),
            V((n_fs, rows, HD), BF16),
            V((n_fs, rows, HV), F32),
            V((n_fs, HD, HV), F32),
            V((n_fs, HD, HD), F32),
            V((n_sp, rows, 2 * HD), BF16),
            V((n_sp, HALF, HD), BF16),
            V((n_sp, HALF, HD), BF16),
            V((n_fs, HD, HV), BF16),
            V((n_fs, HD, HV), BF16),
            V((n_fs, rows, HV), BF16),
            V((2, HALF, HEADS * HD), BF16),
            V((2, HALF, HEADS * HV), BF16),
            dma((22,)),
            dma((12,)),
            dma((12,)),
            dma((3,)),
            dma((3,)),
            dma((n_fs,)),
            dma((n_sp,)),
            dma((n_fs, 2)),
            dma((n_sp,)),
            dma((n_sp // 2,)),
            dma((n_sp,)),
            dma((HEADS,)),
            dma((n_fs, 2)),
            dma((n_fs, 2)),
            dma((n_fs, 2)),
            dma((HEADS,)),
            dma((2,)),
            dma((2,)),
            pltpu.SemaphoreType.REGULAR,
            pltpu.SemaphoreType.REGULAR,
        ],
        compiler_params=pltpu.CompilerParams(
            collective_id=0, has_side_effects=True, vmem_limit_bytes=67043328
        ),
        name="layer",
    )(
        tokens[0],
        norm_gain.reshape(1, -1),
        *flat,
        decay_down.T,
        decay_up.reshape(-1, HD),
        decay_bias,
        log_retain[0].T,
        query_gain.reshape(1, -1),
        key_gain,
        diff_lambda,
        mix_gain.reshape(1, -1),
        state_gain.reshape(1, -1),
        init_state.reshape(n_fs, HD, HV),
        output_attend,
        output_linear,
    )
    return out[None]


def solution(mesh):
    heads = P(None, ("fs", "tp"), None)
    in_specs = (
        P(("grp", "fs"), "sp", None),
        P(),
        heads,
        heads,
        heads,
        heads,
        heads,
        heads,
        P(),
        P(),
        P(),
        P(("grp", "fs"), "sp", None),
        P(),
        P(),
        P(),
        P(),
        P(),
        P("grp", ("fs", "tp"), None, None),
        P(None, "tp"),
        P(None, "tp"),
    )
    out_specs = P(("grp", "fs"), "sp", "tp")
    return jax.shard_map(body, mesh=mesh, in_specs=in_specs, out_specs=out_specs, check_vma=False)
```
